32 devices in a mesh: ep: 8 (over z, y), tp: 4 (over x, core).
Axes of the slice: x: 2, y: 2, z: 4, core: 2. Of those that a mesh axis runs over, the one named last changes fastest.
Arguments:
- mix_input: bfloat16 [8192, 2048], P(('ep', 'tp')), may hold values from -6 to 6
- mix_gain: float32 [2048], replicated, may hold values from 0.1 to 1.9
- pool_weight: bfloat16 [4, 512, 512], replicated, may hold values from -0.25 to 0.25
- pool_scale: float32 [2048], replicated, may hold values from 0.1 to 1.9
- moe_input: bfloat16 [4096, 2048], P(('ep', 'tp')), may hold values from -6 to 6
- moe_gain: float32 [2048], replicated, may hold values from 0.1 to 1.9
- expert_ids: int32 [4096, 4], P('ep'), may hold values from 0 to 15, all different within a row; in each aligned block of 128 rows (0 to 127, 128 to 255, ...) at most 48 rows name the same one
- route_score: float32 [4096, 4], P(('ep', 'tp')), may hold values from 0.05 to 1
- expert_gate: bfloat16 [16, 2048, 1024], P('ep', None, 'tp'), may hold values from -0.125 to 0.125
- expert_up: bfloat16 [16, 2048, 1024], P('ep', None, 'tp'), may hold values from -0.125 to 0.125
- expert_down: bfloat16 [16, 1024, 2048], P('ep', 'tp'), may hold values from -0.1875 to 0.1875
- shared_gate: bfloat16 [2048, 512], P(None, 'tp'), may hold values from -0.125 to 0.125
- shared_up: bfloat16 [2048, 512], P(None, 'tp'), may hold values from -0.125 to 0.125
- shared_down: bfloat16 [512, 2048], P('tp'), may hold values from -0.25 to 0.25
Outputs:
- mix_output: bfloat16 [8192, 2048], P(('ep', 'tp'))
- moe_output: bfloat16 [4096, 2048], P(('ep', 'tp'))
The draws below stay inside these ranges and needn't reach their ends.
Inputs may be any that keep to these rules, and one draw needn't show every extreme that they name: `expert_ids`: each row names 4 different experts. Within each aligned block of 128 rows (the tokens of one device) no expert is named by more than 48 rows, a bound that some block reaches.
All inputs are finite; a program needn't handle non-finite values.
Results may differ from the reference program's by a relative error of at most 0.012.
Values may be sent and summed in bfloat16 or wider, within the bound.
A program may use at most 192 MiB of HBM per device.

```python
import math
import jax
import jax.numpy as jnp
import numpy as np
from jax import lax

D = 2048
GROUP = 512
FF = 1024
SH = 512
EXPERTS = 16
TOPK = 4
TOK_B = 128
TOKENS_A = 8192
TOKENS_B = 4096
CAP = 48
N_TP = 4


def levels(own_key, dims, shards, least, high):
    factor_of = 1.0
    for dim, blocks in shards:
        draws = jax.random.uniform(jax.random.fold_in(jax.random.fold_in(own_key, 6), dim), (blocks,), jnp.float32, least / len(shards), high / len(shards))
        factor_of = factor_of * jnp.repeat(jnp.exp(draws), dims[dim] // blocks).reshape((-1,) + (1,) * (len(dims) - 1 - dim))
    return factor_of


def routed_block(own_key, own, number, rows, amount, top, most, slope):
    order = jax.random.permutation(own_key, amount)
    packed, ordinary = load_shares(amount, rows * top, most, slope, True), load_shares(amount, rows * top, most, slope, False)
    places = jnp.arange(amount)

    def named(sizes, rotation):
        used = int((sizes > 0).sum())
        fixed = max(1, used // 4)
        moved = fixed + (places - fixed + rotation * (used - fixed)) % max(1, amount - fixed)
        return jnp.zeros((amount,), jnp.int32).at[order[jnp.where(places < fixed, places, moved)]].set(jnp.asarray(sizes, jnp.int32))

    sizes = jnp.where(number % 4 == 0, named(packed, number // 4), named(ordinary, number - number // 4 - 1))
    mixed = jax.random.permutation(jax.random.fold_in(own, 3), amount)
    donor, sink = mixed[0:amount // 2 * 2:2], mixed[1:amount // 2 * 2:2]
    margin = jnp.minimum(sizes[donor] - 1, most - sizes[sink]) // 2
    margin = jnp.where((donor == order[0]) | (sink == order[0]) | (sizes[sink] == 0), 0, jnp.maximum(margin, 0))
    moved = jax.random.randint(jax.random.fold_in(own, 4), (amount // 2,), 0, 1 << 20) % (margin + 1)
    sizes = sizes.at[donor].add(-moved).at[sink].add(moved)
    members = jnp.searchsorted(jnp.cumsum(sizes), jnp.arange(rows * top), side="right").astype(jnp.int32)
    listing = members.reshape(top, rows).T
    listing = listing[jax.random.permutation(jax.random.fold_in(own, 1), rows)]
    rotation = jax.random.randint(jax.random.fold_in(own, 2), (rows, 1), 0, top)
    return jnp.take_along_axis(listing, (jnp.arange(top)[None, :] + rotation) % top, axis=1)


def load_shares(amount, total, most, skew, full):
    weights = [(1 << 20) // math.isqrt(standing ** skew) + 1 for standing in range(1, amount + 1)]
    largest = most if full else min(most, max(-(-total // amount), total * weights[0] // sum(weights)))
    least = 1 if total - largest >= amount - 1 else 0
    given, surplus = [largest] + [least] * (amount - 1), total - largest - least * (amount - 1)
    while surplus > 0:
        movable = [i for i in range(1, amount) if given[i] < largest] or [i for i in range(1, amount) if given[i] < most]
        whole, left = sum([weights[i] for i in movable]), surplus
        for i in movable:
            addition = min(most - given[i], max(1, left * weights[i] // whole), surplus)
            given[i] = given[i] + addition
            surplus = surplus - addition
    return np.array(given)


def scatter_about(rng, shape, scale, bound, pieces=(), held_as=jnp.bfloat16):
    entries = scale * jax.random.normal(rng, shape, jnp.float32)
    if pieces:
        entries = entries * levels(rng, shape, pieces, -0.22, 0.18)
    return jnp.clip(entries, -bound, bound).astype(held_as)


def setup_inputs(seed: int = 0) -> dict:
    splits = jax.random.split(jax.random.key(seed), 15)
    mix_input = scatter_about(splits[0], (TOKENS_A, D), 1.0, 6.0, ((0, 32),))
    mix_gain = jnp.clip(1.0 + 0.18 * jax.random.normal(splits[1], (D,), jnp.float32), 0.1, 1.9)
    pool_weight = scatter_about(splits[2], (4, GROUP, GROUP), GROUP ** -0.5, 0.25)
    pool_scale = jnp.clip(1.0 + 0.18 * jax.random.normal(splits[3], (D,), jnp.float32), 0.1, 1.9)
    moe_input = scatter_about(splits[4], (TOKENS_B, D), 1.0, 6.0, ((0, 32),))
    moe_gain = jnp.clip(1.0 + 0.18 * jax.random.normal(splits[5], (D,), jnp.float32), 0.1, 1.9)
    expert_ids_keys = jax.random.split(jax.random.fold_in(splits[6], 1), TOKENS_B // TOK_B)
    expert_ids_turns = jax.random.permutation(jax.random.fold_in(splits[6], 3), TOKENS_B // TOK_B)
    expert_ids = jax.vmap(lambda own, number: routed_block(jax.random.fold_in(splits[6], 2), own, number, TOK_B, EXPERTS, TOPK, CAP, 1))(expert_ids_keys, expert_ids_turns).reshape((TOKENS_B, TOPK))
    route_score = jnp.clip(jnp.exp(math.log(1.0) - 2.9957323 * jax.random.uniform(splits[7], (TOKENS_B, TOPK), jnp.float32) ** levels(splits[7], (TOKENS_B, TOPK), ((0, 32),), -0.2, 0.2)), 0.05, 1.0)
    expert_gate = scatter_about(splits[8], (EXPERTS, D, FF), D ** -0.5, 0.125, ((0, 8), (2, 4)))
    expert_up = scatter_about(splits[9], (EXPERTS, D, FF), D ** -0.5, 0.125, ((0, 8), (2, 4)))
    expert_down = scatter_about(splits[10], (EXPERTS, FF, D), FF ** -0.5, 0.1875, ((0, 8), (1, 4)))
    shared_gate = scatter_about(splits[11], (D, SH), D ** -0.5, 0.125, ((1, 4),))
    shared_up = scatter_about(splits[12], (D, SH), D ** -0.5, 0.125, ((1, 4),))
    shared_down = scatter_about(splits[13], (SH, D), SH ** -0.5, 0.25, ((0, 4),))
    return dict(mix_input=mix_input, mix_gain=mix_gain, pool_weight=pool_weight, pool_scale=pool_scale, moe_input=moe_input, moe_gain=moe_gain, expert_ids=expert_ids, route_score=route_score, expert_gate=expert_gate, expert_up=expert_up, expert_down=expert_down, shared_gate=shared_gate, shared_up=shared_up, shared_down=shared_down)


WINDOWS = (2, 4, 8, 16)
RMS_EPS = 1e-06
ROUTED_SCALE = 2.5

def rms_norm(values, gain_row):
    upcast = values.astype(jnp.float32)
    scaled = upcast * lax.rsqrt(lax.optimization_barrier(jnp.mean(upcast * upcast, axis=-1, keepdims=True)) + RMS_EPS)
    return (scaled * gain_row).astype(jnp.bfloat16)

def rounded(values):
    return lax.optimization_barrier(values.astype(jnp.bfloat16)).astype(jnp.float32)

def window_means(normed, before, offset):
    row_count = normed.shape[0]
    lead_rows = before.shape[0]
    group_size = normed.shape[1] // len(WINDOWS)
    joined = jnp.concatenate([before, normed], axis=0).astype(jnp.float32)
    positions = offset + jnp.arange(row_count, dtype=jnp.int32)
    window_avg = []
    for group_idx, span in enumerate(WINDOWS):
        channels = joined[:, group_idx * group_size:(group_idx + 1) * group_size]
        first_row = lead_rows - span + 1
        running = channels[first_row:first_row + row_count]
        for shift_idx in range(1, span):
            running = running + channels[first_row + shift_idx:first_row + shift_idx + row_count]
        counts = jnp.minimum(positions + 1, span).astype(jnp.float32)
        window_avg.append(running / counts[:, None])
    return jnp.stack(window_avg, axis=1)

def width_sum(hidden, down_rows, block_width):
    summed = jnp.zeros((hidden.shape[0], down_rows.shape[1]), jnp.float32)
    for part_idx in range(N_TP):
        piece_out = jnp.dot(hidden[:, part_idx * block_width:(part_idx + 1) * block_width], down_rows[part_idx * block_width:(part_idx + 1) * block_width], preferred_element_type=jnp.float32)
        summed = summed + rounded(piece_out)
    return summed.astype(jnp.bfloat16)

def reference(mix_input, mix_gain, pool_weight, pool_scale, moe_input, moe_gain, expert_ids, route_score, expert_gate, expert_up, expert_down, shared_gate, shared_up, shared_down):
    normed = rms_norm(mix_input, mix_gain)
    row_count, width_all = normed.shape
    reach_rows = max(WINDOWS) - 1
    before = jnp.zeros((reach_rows, width_all), jnp.bfloat16)
    pooled = window_means(normed, before, 0)
    difference = (pooled - normed.astype(jnp.float32).reshape(row_count, len(WINDOWS), -1)).astype(jnp.bfloat16)
    mixed_out = jnp.einsum('sgc,gcd->sgd', difference.astype(jnp.float32), pool_weight.astype(jnp.float32))
    mix_output = (mixed_out.reshape(row_count, width_all) * pool_scale).astype(jnp.bfloat16)
    tok_count = moe_input.shape[0]
    h_moe = rms_norm(moe_input, moe_gain)
    block_count = tok_count // TOK_B
    pair_ids = expert_ids.reshape(block_count, TOK_B * TOPK)
    onehot = (pair_ids[:, :, None] == jnp.arange(EXPERTS, dtype=jnp.int32)[None, None, :]).astype(jnp.int32)
    rank = lax.optimization_barrier(jnp.sum((jnp.cumsum(onehot, axis=1) - onehot) * onehot, axis=2))
    block_idx = jnp.arange(block_count, dtype=jnp.int32)[:, None]
    slot_col = block_idx * CAP + rank
    owner = block_idx * TOK_B + jnp.arange(TOK_B * TOPK, dtype=jnp.int32)[None, :] // TOPK
    table = jnp.full((EXPERTS, block_count * CAP), tok_count, jnp.int32).at[pair_ids, slot_col].set(owner)
    padded = jnp.concatenate([h_moe, jnp.zeros((1, D), jnp.bfloat16)], axis=0)

    def run_expert(index):
        picked = padded[table[index]]
        gate_val = jnp.dot(picked, expert_gate[index], preferred_element_type=jnp.float32)
        up_val = jnp.dot(picked, expert_up[index], preferred_element_type=jnp.float32)
        hidden = (jax.nn.silu(gate_val) * up_val).astype(jnp.bfloat16)
        return width_sum(hidden, expert_down[index], FF // N_TP)
    results = lax.map(run_expert, jnp.arange(EXPERTS, dtype=jnp.int32))
    flat_res = results.reshape(EXPERTS * block_count * CAP, D)
    flat_idx = (pair_ids * (block_count * CAP) + slot_col).reshape(tok_count, TOPK)
    shared_gate_val = jnp.dot(h_moe, shared_gate, preferred_element_type=jnp.float32)
    shared_up_val = jnp.dot(h_moe, shared_up, preferred_element_type=jnp.float32)
    shared_hidden = (jax.nn.silu(shared_gate_val) * shared_up_val).astype(jnp.bfloat16)
    shared_out = width_sum(shared_hidden, shared_down, SH // N_TP)
    route_w = route_score / lax.optimization_barrier(jnp.sum(route_score, axis=1, keepdims=True)) * ROUTED_SCALE
    combined = shared_out.astype(jnp.float32)
    for pick_idx in range(TOPK):
        combined = combined + route_w[:, pick_idx:pick_idx + 1] * flat_res[flat_idx[:, pick_idx]].astype(jnp.float32)
    return (mix_output, combined.astype(jnp.bfloat16))
```

```python
import jax
import jax.numpy as jnp
from jax import lax
from jax.sharding import PartitionSpec as P

WINDOWS = (2, 4, 8, 16)
RMS_EPS = 1e-06
ROUTED_SCALE = 2.5


def passed_along(value, axis, by):
    length = lax.axis_size(axis)
    pairs = [(i, i + by) for i in range(length) if 0 <= i + by < length]
    return lax.ppermute(value, axis, pairs)


def rms_norm(values, gain_row):
    upcast = values.astype(jnp.float32)
    scaled = upcast * lax.rsqrt(jnp.mean(upcast * upcast, axis=-1, keepdims=True) + RMS_EPS)
    return (scaled * gain_row).astype(jnp.bfloat16)


def rounded(values):
    return lax.optimization_barrier(values.astype(jnp.bfloat16)).astype(jnp.float32)


def window_means(normed, before, offset):
    row_count = normed.shape[0]
    lead_rows = before.shape[0]
    group_size = normed.shape[1] // len(WINDOWS)
    joined = jnp.concatenate([before, normed], axis=0).astype(jnp.float32)
    positions = offset + jnp.arange(row_count, dtype=jnp.int32)
    window_avg = []
    for group_idx, span in enumerate(WINDOWS):
        channels = joined[:, group_idx * group_size : (group_idx + 1) * group_size]
        first_row = lead_rows - span + 1
        running = channels[first_row : first_row + row_count]
        for shift_idx in range(1, span):
            running = running + channels[first_row + shift_idx : first_row + shift_idx + row_count]
        counts = jnp.minimum(positions + 1, span).astype(jnp.float32)
        window_avg.append(running / counts[:, None])
    return jnp.stack(window_avg, axis=1)


def fill_slots(normed, picks, expert_count, capacity):
    tok_count, top_count = picks.shape
    pair_count = tok_count * top_count
    flat_ids = picks.reshape(pair_count)
    matches = flat_ids[:, None] == jnp.arange(expert_count, dtype=jnp.int32)[None, :]
    pair_line = jnp.arange(pair_count, dtype=jnp.int32)
    lower_mask = (pair_line[:, None] > pair_line[None, :]).astype(jnp.bfloat16)
    seen_before = jnp.dot(
        lower_mask, matches.astype(jnp.bfloat16), preferred_element_type=jnp.float32
    )
    rank = jnp.sum(seen_before * matches.astype(jnp.float32), axis=1).astype(jnp.int32)
    slots = flat_ids * capacity + rank
    owner = pair_line // top_count
    slot_token = jnp.full((expert_count * capacity,), tok_count, jnp.int32).at[slots].set(owner)
    padded = jnp.concatenate([normed, jnp.zeros((1, normed.shape[1]), normed.dtype)], axis=0)
    return (padded[slot_token], slots.reshape(tok_count, top_count))


def blockwise_down(hidden, down_rows, pieces, contract):
    block_width = hidden.shape[-1] // pieces
    summed = None
    for part_idx in range(pieces):
        piece_out = jnp.einsum(
            contract,
            hidden[..., part_idx * block_width : (part_idx + 1) * block_width],
            down_rows[..., part_idx * block_width : (part_idx + 1) * block_width, :],
            preferred_element_type=jnp.float32,
        )
        summed = rounded(piece_out) if summed is None else summed + rounded(piece_out)
    return summed.astype(jnp.bfloat16)


def routed_by_slots(h_moe, expert_ids, route_w, expert_gate, expert_up, expert_down, shared_gate, shared_up, shared_down):
    tok_count, model_width = h_moe.shape
    top_count = expert_ids.shape[1]
    quarters = lax.axis_size("tp")
    my_quarter = lax.axis_index("tp")
    ep_count = lax.axis_size("ep")
    local_experts = expert_gate.shape[0]
    expert_count = ep_count * local_experts
    capacity = 3 * tok_count * top_count // (2 * expert_count)
    per_source = local_experts * capacity
    full_gate, full_up, full_down, full_sgate, full_sup, full_sdown = (
        lax.all_gather(expert_gate, "tp", axis=2, tiled=True),
        lax.all_gather(expert_up, "tp", axis=2, tiled=True),
        lax.all_gather(expert_down, "tp", axis=1, tiled=True),
        lax.all_gather(shared_gate, "tp", axis=1, tiled=True),
        lax.all_gather(shared_up, "tp", axis=1, tiled=True),
        lax.all_gather(shared_down, "tp", axis=0, tiled=True),
    )
    my_ids = lax.dynamic_slice_in_dim(expert_ids, my_quarter * tok_count, tok_count, 0)
    outgoing, my_slots = fill_slots(h_moe, my_ids, expert_count, capacity)
    landed = lax.all_to_all(
        outgoing.reshape(ep_count, per_source, model_width),
        "ep",
        split_axis=0,
        concat_axis=0,
        tiled=True,
    )
    routed_in = landed.reshape(ep_count, local_experts, capacity, model_width)
    gate_val = jnp.einsum(
        "necd,edf->necf", routed_in, full_gate, preferred_element_type=jnp.float32
    )
    up_val = jnp.einsum("necd,edf->necf", routed_in, full_up, preferred_element_type=jnp.float32)
    hidden = (jax.nn.silu(gate_val) * up_val).astype(jnp.bfloat16)
    expert_back = blockwise_down(hidden, full_down, quarters, "necf,efd->necd")
    expert_back = expert_back.reshape(ep_count, per_source, model_width)
    shared_gate_val = jnp.dot(h_moe, full_sgate, preferred_element_type=jnp.float32)
    shared_up_val = jnp.dot(h_moe, full_sup, preferred_element_type=jnp.float32)
    shared_hidden = (jax.nn.silu(shared_gate_val) * shared_up_val).astype(jnp.bfloat16)
    shared_back = blockwise_down(shared_hidden, full_sdown, quarters, "tf,fd->td")
    returned = lax.all_to_all(expert_back, "ep", split_axis=0, concat_axis=0, tiled=True)
    returned = returned.reshape(expert_count * capacity, model_width)
    combined = shared_back.astype(jnp.float32)
    for pick_idx in range(top_count):
        combined = combined + route_w[:, pick_idx : pick_idx + 1] * returned[
            my_slots[:, pick_idx]
        ].astype(jnp.float32)
    return combined.astype(jnp.bfloat16)


def plus(mine, arrived):
    return (mine.astype(jnp.float32) + arrived.astype(jnp.float32)).astype(jnp.bfloat16)


def routed_by_sums(h_moe, expert_ids, route_w, expert_gate, expert_up, expert_down, shared_gate, shared_up, shared_down):
    tok_count, model_width = h_moe.shape
    half_width = model_width // 2
    ep_count, tp_count = lax.axis_size("ep"), lax.axis_size("tp")
    z_count, x_count = ep_count // 2, tp_count // 2
    my_ep, my_tp = lax.axis_index("ep"), lax.axis_index("tp")
    my_z, my_y, my_x, my_core = my_ep // 2, my_ep % 2, my_tp // 2, my_tp % 2
    local_experts, _, width = expert_gate.shape
    expert_count = ep_count * local_experts

    def over_core(value):
        return lax.ppermute(value, "tp", [(i, i ^ 1) for i in range(tp_count)])

    def over_x(value):
        return lax.ppermute(value, "tp", [(i, (i + 2) % tp_count) for i in range(tp_count)])

    def over_y(value):
        return lax.ppermute(value, "ep", [(i, i ^ 1) for i in range(ep_count)])

    def over_z(value):
        return lax.ppermute(value, "ep", [(i, (i + 2) % ep_count) for i in range(ep_count)])

    def both(weight, axis):
        return jnp.concatenate([weight, over_core(weight)], axis=axis)

    my_ids = lax.dynamic_slice_in_dim(expert_ids, my_tp * tok_count, tok_count, 0)
    share = jnp.zeros((expert_count, tok_count), jnp.float32)
    for pick_idx in range(expert_ids.shape[1]):
        named = my_ids[None, :, pick_idx] == jnp.arange(expert_count, dtype=jnp.int32)[:, None]
        share = share + jnp.where(named, route_w[None, :, pick_idx], 0.0)
    all_share = lax.all_gather(share, ("ep", "tp"), axis=0, tiled=False)
    my_share = lax.dynamic_slice_in_dim(all_share, my_ep * local_experts, local_experts, 1)

    ring = [(h_moe[:, :half_width], h_moe[:, half_width:])]
    for _ in range(z_count - 1):
        ring.append((over_z(ring[-1][0]), over_z(ring[-1][1])))

    gate_cols = both(expert_gate, 2)
    up_cols = both(expert_up, 2)
    down_rows = both(expert_down, 1).reshape(local_experts * 2 * width, model_width)
    sgate_cols, sup_cols, sdown_rows = both(shared_gate, 1), both(shared_up, 1), both(shared_down, 0)

    homes = []
    for step in range(z_count):
        left, right = ring[step]
        left = jnp.concatenate([left, over_y(left)], axis=0)
        left = jnp.concatenate([left, over_x(left)], axis=0)
        right_x = over_x(right)
        right_pair = over_y(jnp.concatenate([right, right_x], axis=0))
        right = jnp.concatenate(
            [right, right_pair[:tok_count], right_x, right_pair[tok_count:]], axis=0
        )
        rows = jnp.concatenate([left, right], axis=1)
        weights = []
        for dx in range(2):
            for dy in range(2):
                source_ep = (my_z - step) % z_count * 2 + (my_y + dy) % 2
                source_tp = (my_x + dx) % x_count * 2 + my_core
                weights.append(
                    lax.dynamic_index_in_dim(
                        my_share, source_ep * tp_count + source_tp, 0, keepdims=False
                    )
                )
        weights = jnp.concatenate(weights, axis=1)
        hidden = []
        for local in range(local_experts):
            gate_val = jnp.dot(rows, gate_cols[local], preferred_element_type=jnp.float32)
            up_val = jnp.dot(rows, up_cols[local], preferred_element_type=jnp.float32)
            weight = weights[local][:, None]
            hidden.append(
                jnp.where(weight > 0, jax.nn.silu(gate_val) * up_val * weight, 0.0).astype(
                    jnp.bfloat16
                )
            )
        result = jnp.dot(
            jnp.concatenate(hidden, axis=1), down_rows, preferred_element_type=jnp.float32
        )
        if step == 0:
            blocks = [result[i * tok_count : (i + 1) * tok_count] for i in range(4)]
            own = jnp.concatenate([rows[:tok_count], rows[2 * tok_count : 3 * tok_count]], axis=0)
            shared_gate_val = jnp.dot(own, sgate_cols, preferred_element_type=jnp.float32)
            shared_up_val = jnp.dot(own, sup_cols, preferred_element_type=jnp.float32)
            shared_hidden = (jax.nn.silu(shared_gate_val) * shared_up_val).astype(jnp.bfloat16)
            shared_part = jnp.dot(shared_hidden, sdown_rows, preferred_element_type=jnp.float32)
            result = jnp.concatenate(
                [
                    blocks[0] + shared_part[:tok_count],
                    blocks[1],
                    blocks[2] + shared_part[tok_count:],
                    blocks[3],
                ],
                axis=0,
            )
        result = result.astype(jnp.bfloat16).reshape(2, 2, tok_count, model_width)
        left, right = result[..., :half_width], result[..., half_width:]
        left = plus(left[0], over_x(left[1]))
        left = plus(left[0], over_y(left[1]))
        right = plus(right[:, 0], over_y(right[:, 1]))
        right = plus(right[0], over_x(right[1]))
        homes.append((left, right))
    total = homes[1]
    for step in range(2, z_count + 1):
        here = homes[step % z_count]
        total = (plus(here[0], over_z(total[0])), plus(here[1], over_z(total[1])))
    return jnp.concatenate(total, axis=1)


def per_device(
    mix_input,
    mix_gain,
    pool_weight,
    pool_scale,
    moe_input,
    moe_gain,
    expert_ids,
    route_score,
    expert_gate,
    expert_up,
    expert_down,
    shared_gate,
    shared_up,
    shared_down,
):
    normed = rms_norm(mix_input, mix_gain)
    row_count, width_all = normed.shape
    reach_rows = max(WINDOWS) - 1
    before = passed_along(normed[row_count - reach_rows :], ("ep", "tp"), 1)
    offset = lax.axis_index(("ep", "tp")) * row_count
    pooled = window_means(normed, before, offset)
    difference = (pooled - normed.astype(jnp.float32).reshape(row_count, len(WINDOWS), -1)).astype(
        jnp.bfloat16
    )
    mixed_out = jnp.einsum(
        "sgc,gcd->sgd", difference, pool_weight, preferred_element_type=jnp.float32
    )
    mix_output = (mixed_out.reshape(row_count, width_all) * pool_scale).astype(jnp.bfloat16)
    h_moe = rms_norm(moe_input, moe_gain)
    route_w = route_score / jnp.sum(route_score, axis=1, keepdims=True) * ROUTED_SCALE
    ep_count, tp_count = lax.axis_size("ep"), lax.axis_size("tp")
    few_experts = (
        ep_count * expert_gate.shape[0] <= 8 * expert_ids.shape[1]
        and ep_count % 2 == 0
        and ep_count > 2
        and tp_count == 4
    )
    run_experts = routed_by_sums if few_experts else routed_by_slots
    moe_output = run_experts(
        h_moe,
        expert_ids,
        route_w,
        expert_gate,
        expert_up,
        expert_down,
        shared_gate,
        shared_up,
        shared_down,
    )
    return (mix_output, moe_output)


def solution(mesh):
    return jax.shard_map(
        per_device,
        mesh=mesh,
        in_specs=(
            P(("ep", "tp"), None),
            P(),
            P(),
            P(),
            P(("ep", "tp"), None),
            P(),
            P("ep", None),
            P(("ep", "tp"), None),
            P("ep", None, "tp"),
            P("ep", None, "tp"),
            P("ep", "tp", None),
            P(None, "tp"),
            P(None, "tp"),
            P("tp", None),
        ),
        out_specs=(P(("ep", "tp"), None), P(("ep", "tp"), None)),
        check_vma=False,
    )
```

```python
import jax
import jax.numpy as jnp
from jax import lax
from jax.sharding import PartitionSpec as P

WINDOWS = (2, 4, 8, 16)
RMS_EPS = 1e-06
ROUTED_SCALE = 2.5


def passed_along(value, axis, by):
    length = lax.axis_size(axis)
    pairs = [(i, i + by) for i in range(length) if 0 <= i + by < length]
    return lax.ppermute(value, axis, pairs)


def rms_norm(values, gain_row):
    upcast = values.astype(jnp.float32)
    scaled = upcast * lax.rsqrt(jnp.mean(upcast * upcast, axis=-1, keepdims=True) + RMS_EPS)
    return (scaled * gain_row).astype(jnp.bfloat16)


def rounded(values):
    return lax.optimization_barrier(values.astype(jnp.bfloat16)).astype(jnp.float32)


def window_means(normed, before, offset):
    row_count = normed.shape[0]
    lead_rows = before.shape[0]
    group_size = normed.shape[1] // len(WINDOWS)
    joined = jnp.concatenate([before, normed], axis=0).astype(jnp.float32)
    positions = offset + jnp.arange(row_count, dtype=jnp.int32)
    window_avg = []
    for group_idx, span in enumerate(WINDOWS):
        channels = joined[:, group_idx * group_size : (group_idx + 1) * group_size]
        first_row = lead_rows - span + 1
        running = channels[first_row : first_row + row_count]
        for shift_idx in range(1, span):
            running = running + channels[first_row + shift_idx : first_row + shift_idx + row_count]
        counts = jnp.minimum(positions + 1, span).astype(jnp.float32)
        window_avg.append(running / counts[:, None])
    return jnp.stack(window_avg, axis=1)


def fill_slots(normed, picks, expert_count, capacity):
    tok_count, top_count = picks.shape
    pair_count = tok_count * top_count
    flat_ids = picks.reshape(pair_count)
    matches = flat_ids[:, None] == jnp.arange(expert_count, dtype=jnp.int32)[None, :]
    pair_line = jnp.arange(pair_count, dtype=jnp.int32)
    lower_mask = (pair_line[:, None] > pair_line[None, :]).astype(jnp.bfloat16)
    seen_before = jnp.dot(
        lower_mask, matches.astype(jnp.bfloat16), preferred_element_type=jnp.float32
    )
    rank = jnp.sum(seen_before * matches.astype(jnp.float32), axis=1).astype(jnp.int32)
    slots = flat_ids * capacity + rank
    owner = pair_line // top_count
    slot_token = jnp.full((expert_count * capacity,), tok_count, jnp.int32).at[slots].set(owner)
    padded = jnp.concatenate([normed, jnp.zeros((1, normed.shape[1]), normed.dtype)], axis=0)
    return (padded[slot_token], slots.reshape(tok_count, top_count))


def blockwise_down(hidden, down_rows, pieces, contract):
    block_width = hidden.shape[-1] // pieces
    summed = None
    for part_idx in range(pieces):
        piece_out = jnp.einsum(
            contract,
            hidden[..., part_idx * block_width : (part_idx + 1) * block_width],
            down_rows[..., part_idx * block_width : (part_idx + 1) * block_width, :],
            preferred_element_type=jnp.float32,
        )
        summed = rounded(piece_out) if summed is None else summed + rounded(piece_out)
    return summed.astype(jnp.bfloat16)


def routed_by_slots(h_moe, expert_ids, route_w, expert_gate, expert_up, expert_down, shared_gate, shared_up, shared_down):
    tok_count, model_width = h_moe.shape
    top_count = expert_ids.shape[1]
    quarters = lax.axis_size("tp")
    my_quarter = lax.axis_index("tp")
    ep_count = lax.axis_size("ep")
    local_experts = expert_gate.shape[0]
    expert_count = ep_count * local_experts
    capacity = 3 * tok_count * top_count // (2 * expert_count)
    per_source = local_experts * capacity
    full_gate, full_up, full_down, full_sgate, full_sup, full_sdown = (
        lax.all_gather(expert_gate, "tp", axis=2, tiled=True),
        lax.all_gather(expert_up, "tp", axis=2, tiled=True),
        lax.all_gather(expert_down, "tp", axis=1, tiled=True),
        lax.all_gather(shared_gate, "tp", axis=1, tiled=True),
        lax.all_gather(shared_up, "tp", axis=1, tiled=True),
        lax.all_gather(shared_down, "tp", axis=0, tiled=True),
    )
    my_ids = lax.dynamic_slice_in_dim(expert_ids, my_quarter * tok_count, tok_count, 0)
    outgoing, my_slots = fill_slots(h_moe, my_ids, expert_count, capacity)
    landed = lax.all_to_all(
        outgoing.reshape(ep_count, per_source, model_width),
        "ep",
        split_axis=0,
        concat_axis=0,
        tiled=True,
    )
    routed_in = landed.reshape(ep_count, local_experts, capacity, model_width)
    gate_val = jnp.einsum(
        "necd,edf->necf", routed_in, full_gate, preferred_element_type=jnp.float32
    )
    up_val = jnp.einsum("necd,edf->necf", routed_in, full_up, preferred_element_type=jnp.float32)
    hidden = (jax.nn.silu(gate_val) * up_val).astype(jnp.bfloat16)
    expert_back = blockwise_down(hidden, full_down, quarters, "necf,efd->necd")
    expert_back = expert_back.reshape(ep_count, per_source, model_width)
    shared_gate_val = jnp.dot(h_moe, full_sgate, preferred_element_type=jnp.float32)
    shared_up_val = jnp.dot(h_moe, full_sup, preferred_element_type=jnp.float32)
    shared_hidden = (jax.nn.silu(shared_gate_val) * shared_up_val).astype(jnp.bfloat16)
    shared_back = blockwise_down(shared_hidden, full_sdown, quarters, "tf,fd->td")
    returned = lax.all_to_all(expert_back, "ep", split_axis=0, concat_axis=0, tiled=True)
    returned = returned.reshape(expert_count * capacity, model_width)
    combined = shared_back.astype(jnp.float32)
    for pick_idx in range(top_count):
        combined = combined + route_w[:, pick_idx : pick_idx + 1] * returned[
            my_slots[:, pick_idx]
        ].astype(jnp.float32)
    return combined.astype(jnp.bfloat16)


def plus(mine, arrived):
    return (mine.astype(jnp.float32) + arrived.astype(jnp.float32)).astype(jnp.bfloat16)


def routed_by_sums(h_moe, expert_ids, route_w, expert_gate, expert_up, expert_down, shared_gate, shared_up, shared_down):
    tok_count, model_width = h_moe.shape
    half_width = model_width // 2
    ep_count, tp_count = lax.axis_size("ep"), lax.axis_size("tp")
    z_count, x_count = ep_count // 2, tp_count // 2
    my_ep, my_tp = lax.axis_index("ep"), lax.axis_index("tp")
    my_z, my_y, my_x, my_core = my_ep // 2, my_ep % 2, my_tp // 2, my_tp % 2
    local_experts, _, width = expert_gate.shape
    expert_count = ep_count * local_experts

    def over_core(value):
        return lax.ppermute(value, "tp", [(i, i ^ 1) for i in range(tp_count)])

    def over_x(value):
        return lax.ppermute(value, "tp", [(i, (i + 2) % tp_count) for i in range(tp_count)])

    def over_y(value):
        return lax.ppermute(value, "ep", [(i, i ^ 1) for i in range(ep_count)])

    def over_z(value):
        return lax.ppermute(value, "ep", [(i, (i + 2) % ep_count) for i in range(ep_count)])

    def both(weight, axis):
        return jnp.concatenate([weight, over_core(weight)], axis=axis)

    my_ids = lax.dynamic_slice_in_dim(expert_ids, my_tp * tok_count, tok_count, 0)
    share = jnp.zeros((expert_count, tok_count), jnp.float32)
    for pick_idx in range(expert_ids.shape[1]):
        named = my_ids[None, :, pick_idx] == jnp.arange(expert_count, dtype=jnp.int32)[:, None]
        share = share + jnp.where(named, route_w[None, :, pick_idx], 0.0)
    all_share = lax.all_gather(share, ("ep", "tp"), axis=0, tiled=False)
    my_share = lax.dynamic_slice_in_dim(all_share, my_ep * local_experts, local_experts, 1)

    h_moe, my_share, expert_gate, expert_up, expert_down = lax.optimization_barrier(
        (h_moe, my_share, expert_gate, expert_up, expert_down)
    )
    ring = [(h_moe[:, :half_width], h_moe[:, half_width:])]
    for _ in range(z_count - 1):
        ring.append((over_z(ring[-1][0]), over_z(ring[-1][1])))

    gate_cols = both(expert_gate, 2)
    up_cols = both(expert_up, 2)
    down_rows = both(expert_down, 1).reshape(local_experts * 2 * width, model_width)
    sgate_cols, sup_cols, sdown_rows = both(shared_gate, 1), both(shared_up, 1), both(shared_down, 0)

    homes = []
    for step in range(z_count):
        left, right = ring[step]
        left = jnp.concatenate([left, over_y(left)], axis=0)
        left = jnp.concatenate([left, over_x(left)], axis=0)
        right_x = over_x(right)
        right_pair = over_y(jnp.concatenate([right, right_x], axis=0))
        right = jnp.concatenate(
            [right, right_pair[:tok_count], right_x, right_pair[tok_count:]], axis=0
        )
        rows = jnp.concatenate([left, right], axis=1)
        weights = []
        for dx in range(2):
            for dy in range(2):
                source_ep = (my_z - step) % z_count * 2 + (my_y + dy) % 2
                source_tp = (my_x + dx) % x_count * 2 + my_core
                weights.append(
                    lax.dynamic_index_in_dim(
                        my_share, source_ep * tp_count + source_tp, 0, keepdims=False
                    )
                )
        weights = jnp.concatenate(weights, axis=1).T
        if step >= 2:
            rows, homes[step - 2] = lax.optimization_barrier((rows, homes[step - 2]))
        hidden = []
        for local in range(local_experts):
            gate_val = jnp.dot(rows, gate_cols[local], preferred_element_type=jnp.float32)
            up_val = jnp.dot(rows, up_cols[local], preferred_element_type=jnp.float32)
            weight = weights[:, local : local + 1]
            hidden.append((jax.nn.silu(gate_val) * up_val * weight).astype(jnp.bfloat16))
        result = jnp.dot(
            jnp.concatenate(hidden, axis=1), down_rows, preferred_element_type=jnp.float32
        )
        if step == 0:
            blocks = [result[i * tok_count : (i + 1) * tok_count] for i in range(4)]
            own = jnp.concatenate([rows[:tok_count], rows[2 * tok_count : 3 * tok_count]], axis=0)
            shared_gate_val = jnp.dot(own, sgate_cols, preferred_element_type=jnp.float32)
            shared_up_val = jnp.dot(own, sup_cols, preferred_element_type=jnp.float32)
            shared_hidden = (jax.nn.silu(shared_gate_val) * shared_up_val).astype(jnp.bfloat16)
            shared_part = jnp.dot(shared_hidden, sdown_rows, preferred_element_type=jnp.float32)
            result = jnp.concatenate(
                [
                    blocks[0] + shared_part[:tok_count],
                    blocks[1],
                    blocks[2] + shared_part[tok_count:],
                    blocks[3],
                ],
                axis=0,
            )
        result = result.astype(jnp.bfloat16).reshape(2, 2, tok_count, model_width)
        left, right = result[..., :half_width], result[..., half_width:]
        left = plus(left[0], over_x(left[1]))
        left = plus(left[0], over_y(left[1]))
        right = plus(right[:, 0], over_y(right[:, 1]))
        right = plus(right[0], over_x(right[1]))
        homes.append((left, right))
    total = homes[1]
    for step in range(2, z_count + 1):
        here = homes[step % z_count]
        total = (plus(here[0], over_z(total[0])), plus(here[1], over_z(total[1])))
    return jnp.concatenate(total, axis=1)


def per_device(
    mix_input,
    mix_gain,
    pool_weight,
    pool_scale,
    moe_input,
    moe_gain,
    expert_ids,
    route_score,
    expert_gate,
    expert_up,
    expert_down,
    shared_gate,
    shared_up,
    shared_down,
):
    normed = rms_norm(mix_input, mix_gain)
    row_count, width_all = normed.shape
    reach_rows = max(WINDOWS) - 1
    before = passed_along(normed[row_count - reach_rows :], ("ep", "tp"), 1)
    offset = lax.axis_index(("ep", "tp")) * row_count
    pooled = window_means(normed, before, offset)
    difference = (pooled - normed.astype(jnp.float32).reshape(row_count, len(WINDOWS), -1)).astype(
        jnp.bfloat16
    )
    mixed_out = jnp.einsum(
        "sgc,gcd->sgd", difference, pool_weight, preferred_element_type=jnp.float32
    )
    mix_output = (mixed_out.reshape(row_count, width_all) * pool_scale).astype(jnp.bfloat16)
    h_moe = rms_norm(moe_input, moe_gain)
    route_w = route_score / jnp.sum(route_score, axis=1, keepdims=True) * ROUTED_SCALE
    ep_count, tp_count = lax.axis_size("ep"), lax.axis_size("tp")
    few_experts = (
        ep_count * expert_gate.shape[0] <= 8 * expert_ids.shape[1]
        and ep_count % 2 == 0
        and ep_count > 2
        and tp_count == 4
    )
    run_experts = routed_by_sums if few_experts else routed_by_slots
    moe_output = run_experts(
        h_moe,
        expert_ids,
        route_w,
        expert_gate,
        expert_up,
        expert_down,
        shared_gate,
        shared_up,
        shared_down,
    )
    return (mix_output, moe_output)


def solution(mesh):
    return jax.shard_map(
        per_device,
        mesh=mesh,
        in_specs=(
            P(("ep", "tp"), None),
            P(),
            P(),
            P(),
            P(("ep", "tp"), None),
            P(),
            P("ep", None),
            P(("ep", "tp"), None),
            P("ep", None, "tp"),
            P("ep", None, "tp"),
            P("ep", "tp", None),
            P(None, "tp"),
            P(None, "tp"),
            P("tp", None),
        ),
        out_specs=(P(("ep", "tp"), None), P(("ep", "tp"), None)),
        check_vma=False,
    )
```
